32 devices in a mesh: gr: 2 (over y), sp: 4 (over z), tp: 4 (over x, core).
Axes of the slice: x: 2, y: 2, z: 4, core: 2. Of those that a mesh axis runs over, the one named last changes fastest.
Arguments:
- layer_input: bfloat16 [2, 3072, 2048], P('gr', ('sp', 'tp')), may hold values from -6 to 6
- key_weight: bfloat16 [2048, 2048], P(None, 'tp'), may hold values from -0.125 to 0.125
- value_weight: bfloat16 [2048, 2048], P(None, 'tp'), may hold values from -0.125 to 0.125
- new_queries: bfloat16 [2, 2048], P('gr', 'tp'), may hold values from -280 to 280
- lambdas: float32 [16], P('tp'), may hold values from 0.3 to 0.8
- head_gain: float32 [128], replicated, may hold values from 0.1 to 1.9
- out_weight: bfloat16 [2048, 2048], P('tp'), may hold values from -0.125 to 0.125
Outputs:
- key_cache: bfloat16 [2, 3072, 2048], P('gr', 'sp', 'tp')
- value_cache: bfloat16 [2, 3072, 2048], P('gr', 'sp', 'tp')
- mixed: bfloat16 [2, 2048], P('gr', 'tp')
The draws below stay inside these ranges and needn't reach their ends.
All inputs are finite; a program needn't handle non-finite values.
Results may differ from the reference program's by a relative error of at most 0.03.
Values may be sent and summed in bfloat16 or wider, within the bound.
No kernel may reach another device: no remote copies, remote signals or barrier semaphores. Data moves between devices by JAX's collectives and lax.ppermute only.
A program may use at most 64 MiB of HBM per device.

```python
import jax
import jax.numpy as jnp
from jax import lax

D = 2048
HEADS = 16
HEAD_DIM = 64
ROWS = 192
LEN = 3072
SEQS = 2
N_SP = 4
N_TP = 4


def draw_new_queries(key, part):
    drawn_rows = jax.random.normal(jax.random.fold_in(key, 11), (SEQS, HEADS * 2 * HEAD_DIM), jnp.float32)
    drawn_rows = jnp.clip(drawn_rows, -4.0, 4.0) * 1.7
    return drawn_rows.astype(jnp.bfloat16)


def block_scale(key, shape, pieces, low, high):
    factor_of, own = 1.0, jax.random.fold_in(key, 6)
    for position, parts in pieces:
        heights = jnp.exp(jax.random.uniform(jax.random.fold_in(own, position), (parts,), jnp.float32, low / len(pieces), high / len(pieces)))
        factor_of = factor_of * jnp.repeat(heights, shape[position] // parts).reshape([-1 if axis == position else 1 for axis in range(len(shape))])
    return factor_of


def gaussian(own_key, dims, scale, most, cuts=(), kind=jnp.bfloat16):
    loudness = block_scale(own_key, dims, cuts, -0.22, 0.18) if cuts else 1.0
    entries = jax.random.normal(own_key, dims, jnp.float32) * scale * loudness
    return jnp.minimum(jnp.maximum(entries, -most), most).astype(kind)


def setup_inputs(seed: int = 0) -> dict:
    arg_keys = jax.random.split(jax.random.key(seed), 8)
    return {
        "layer_input": gaussian(arg_keys[0], (SEQS, LEN, D), 1.0, 6.0, ((0, 2), (1, 16))),
        "key_weight": gaussian(arg_keys[1], (D, HEADS * 2 * HEAD_DIM), D ** -0.5, 0.125, ((1, 4),)),
        "value_weight": gaussian(arg_keys[2], (D, HEADS * 2 * HEAD_DIM), D ** -0.5, 0.125, ((1, 4),)),
        "new_queries": draw_new_queries(jax.random.fold_in(arg_keys[7], 71), 0),
        "lambdas": jnp.clip(0.3 + 0.5 * jax.random.uniform(arg_keys[4], (HEADS,), jnp.float32) ** block_scale(arg_keys[4], (HEADS,), ((0, 4),), -0.2, 0.2), 0.3, 0.8),
        "head_gain": jnp.clip(1.0 + 0.18 * jax.random.normal(arg_keys[5], (2 * HEAD_DIM,), jnp.float32), 0.1, 1.9),
        "out_weight": gaussian(arg_keys[6], (HEADS * 2 * HEAD_DIM, D), (HEADS * 2 * HEAD_DIM) ** -0.5, 0.125, ((0, 4),)),
    }


def rotate(raw_keys, positions, head_dim):
    inverse = 1.0 / 10000.0 ** (jnp.arange(0, head_dim, 2, dtype=jnp.float32) / head_dim)
    angles = positions.astype(jnp.float32)[:, None] * inverse[None, :]
    angles = jnp.concatenate([angles, angles], axis=-1)
    cosine = jnp.cos(angles)[:, None, :]
    sine = jnp.sin(angles)[:, None, :]
    first_half, second_half = jnp.split(raw_keys, 2, axis=-1)
    turned = jnp.concatenate([-second_half, first_half], axis=-1)
    return raw_keys * cosine + turned * sine

def reference(layer_input, key_weight, value_weight, new_queries, lambdas, head_gain, out_weight):
    block_rows = ROWS * N_TP
    column_count = HEADS * 2 * HEAD_DIM

    def project(items):
        block, index = items
        raw_keys = jnp.dot(block, key_weight, preferred_element_type=jnp.float32)
        raw_keys = raw_keys.reshape(block_rows, 2 * HEADS, HEAD_DIM)
        positions = index * block_rows + jnp.arange(block_rows, dtype=jnp.int32)
        key_rows = rotate(raw_keys, positions, HEAD_DIM)
        key_rows = key_rows.reshape(block_rows, column_count).astype(jnp.bfloat16)
        value_rows = jnp.dot(block, value_weight, preferred_element_type=jnp.float32).astype(jnp.bfloat16)
        return (key_rows, value_rows)
    key_list = []
    value_list = []
    read_list = []
    for seq_index in range(SEQS):
        blocks = layer_input[seq_index].reshape(N_SP, block_rows, D)
        key_blocks, value_blocks = lax.map(project, (blocks, jnp.arange(N_SP, dtype=jnp.int32)))
        key_rows = key_blocks.reshape(LEN, column_count)
        value_rows = value_blocks.reshape(LEN, column_count)
        query_row = new_queries[seq_index].astype(jnp.float32)

        def read_head(head):
            first = (head * 2 * HEAD_DIM).astype(jnp.int32)
            key_part = lax.dynamic_slice_in_dim(key_rows, first, 2 * HEAD_DIM, 1).astype(jnp.float32)
            key_part = key_part.reshape(LEN, 2, HEAD_DIM)
            value_part = lax.dynamic_slice_in_dim(value_rows, first, 2 * HEAD_DIM, 1).astype(jnp.float32)
            query_part = lax.dynamic_slice_in_dim(query_row, first, 2 * HEAD_DIM, 0).reshape(2, HEAD_DIM)
            scores = jnp.einsum('md,lmd->ml', query_part, key_part) * HEAD_DIM ** (-0.5)
            maps = jax.nn.softmax(scores, axis=-1)
            return jnp.einsum('ml,le->me', maps, value_part)
        read_list.append(lax.map(read_head, jnp.arange(HEADS, dtype=jnp.int32)))
        key_list.append(key_rows)
        value_list.append(value_rows)
    key_cache = jnp.stack(key_list, axis=0)
    value_cache = jnp.stack(value_list, axis=0)
    reads = jnp.stack(read_list, axis=0)
    diff = reads[:, :, 0] - lambdas[None, :, None] * reads[:, :, 1]
    normed = diff * lax.rsqrt(lax.optimization_barrier(jnp.mean(diff * diff, axis=-1, keepdims=True)) + 1e-06) * head_gain
    headed = normed.reshape(SEQS, column_count).astype(jnp.bfloat16)
    group_cols = column_count // N_TP
    grouped = headed.reshape(SEQS, N_TP, group_cols).astype(jnp.float32)
    weight_groups = out_weight.reshape(N_TP, group_cols, D).astype(jnp.float32)
    partials = jnp.einsum('stc,tcd->std', grouped, weight_groups).astype(jnp.bfloat16)
    mixed = lax.optimization_barrier(jnp.sum(partials.astype(jnp.float32), axis=1)).astype(jnp.bfloat16)
    return (key_cache, value_cache, mixed)
```

```python
import functools

import jax
import jax.numpy as jnp
from jax import lax
from jax.experimental import pallas as pl
from jax.experimental.pallas import tpu as pltpu
from jax.sharding import PartitionSpec as P


LANES = 128
F32 = jnp.float32
BF16 = jnp.bfloat16


def rope_table(first_position, count, head_dim):
    inverse = 1.0 / 10000.0 ** (jnp.arange(0, head_dim, 2, dtype=F32) / head_dim)
    positions = first_position + jnp.arange(count, dtype=jnp.int32)
    angles = positions.astype(F32)[:, None] * inverse[None, :]
    cosine, sine = jnp.cos(angles), jnp.sin(angles)
    return jnp.concatenate([cosine, cosine, -sine, sine], axis=-1)


def turn(rows, table, head_dim):
    half = head_dim // 2
    lane = lax.broadcasted_iota(jnp.int32, rows.shape, 1)
    swapped = pltpu.roll(table, head_dim, 1)
    low = lane < head_dim
    cosine = jnp.where(low, table, swapped)
    sine = jnp.where(low, swapped, table)
    left = pltpu.roll(rows, LANES - half, 1)
    right = pltpu.roll(rows, half, 1)
    turned = jnp.where(lane % head_dim < half, left, right)
    return rows * cosine + turned * sine


def project_kernel(pieces, heads, head_dim, tile, first, *refs):
    count = len(pieces)
    x_refs, refs = refs[:count], refs[count:]
    wk_ref, wv_ref, q_ref, table_ref, refs = refs[0], refs[1], refs[2], refs[3], refs[4:]
    if not first:
        before_ref, refs = refs[0], refs[3:]
    k_out, v_out, state_ref, xs, wbuf, kbuf, vbuf, x_sem, w_sem, o_sem = refs
    me = lax.axis_index("tp")
    block_rows = pieces[0][3]
    columns = wk_ref.shape[1]
    tiles = columns // tile
    lengths = [piece[2] for piece in pieces]
    starts = [sum(lengths[:i]) for i in range(count)]
    total = sum(lengths)
    offsets = [
        pl.multiple_of(source(me) * block_rows + row, 16) for source, row, _, _ in pieces
    ]
    x_copies = [
        pltpu.make_async_copy(x_refs[i], xs.at[pl.ds(starts[i], lengths[i])], x_sem.at[i])
        for i in range(count)
    ]
    w_copies = [
        pltpu.make_async_copy(
            (wk_ref if t < tiles else wv_ref).at[:, pl.ds((t % tiles) * tile, tile)],
            wbuf.at[t],
            w_sem.at[t],
        )
        for t in range(2 * tiles)
    ]
    for copy in x_copies:
        copy.start()
    for copy in w_copies:
        copy.start()
    for copy in x_copies:
        copy.wait()
    group = total if total <= 256 else lengths[0]
    spans = [(r, min(group, total - r)) for r in range(0, total, group)]
    tables = [table_ref[pl.ds(offsets[i], lengths[i]), :] for i in range(count)]
    table = tables[0] if count == 1 else jnp.concatenate(tables, axis=0)
    for t in range(2 * tiles):
        w_copies[t].wait()
        for row, length in spans:
            raw = jnp.dot(xs[pl.ds(row, length), :], wbuf[t], preferred_element_type=F32)
            if t < tiles:
                for c in range(0, tile, LANES):
                    turned = turn(raw[:, c : c + LANES], table[row : row + length], head_dim)
                    kbuf[pl.ds(row, length), pl.ds(t * tile + c, LANES)] = turned.astype(BF16)
            else:
                vbuf[pl.ds(row, length), pl.ds((t - tiles) * tile, tile)] = raw.astype(BF16)
        if t == tiles - 1:
            k_writes = [
                pltpu.make_async_copy(
                    kbuf.at[pl.ds(starts[i], lengths[i])],
                    k_out.at[pl.ds(offsets[i], lengths[i])],
                    o_sem.at[i],
                )
                for i in range(count)
            ]
            for copy in k_writes:
                copy.start()
    v_writes = [
        pltpu.make_async_copy(
            vbuf.at[pl.ds(starts[i], lengths[i])],
            v_out.at[pl.ds(offsets[i], lengths[i])],
            o_sem.at[count + i],
        )
        for i in range(count)
    ]
    for copy in v_writes:
        copy.start()

    lines = state_ref.shape[0] // 3
    line = lax.broadcasted_iota(jnp.int32, (lines, columns), 0)
    lane = lax.broadcasted_iota(jnp.int32, (lines, columns), 1)
    mine = lane // head_dim == (line % heads) * 2 + line // heads
    spread = jnp.broadcast_to(q_ref[...].astype(F32), (lines, columns))
    queries = jnp.where(mine, spread, 0.0).astype(BF16)
    scores = lax.dot_general(
        queries, kbuf[...], (((1,), (1,)), ((), ())), preferred_element_type=F32
    )
    scores = scores * head_dim ** (-0.5)
    highest = jnp.max(scores, axis=1, keepdims=True)
    if not first:
        earlier = before_ref[pl.ds(lines, lines), :][:, :1]
        highest = jnp.maximum(highest, earlier)
    weights = jnp.exp(scores - highest)
    totals = jnp.sum(weights, axis=1, keepdims=True)
    coarse = weights.astype(BF16)
    fine = (weights - coarse.astype(F32)).astype(BF16)
    values = vbuf[...]
    wide = jnp.dot(coarse, values, preferred_element_type=F32)
    wide = wide + jnp.dot(fine, values, preferred_element_type=F32)
    row_id = lax.broadcasted_iota(jnp.int32, (lines, 2 * head_dim), 0)
    weighted = jnp.zeros((lines, 2 * head_dim), F32)
    for h in range(heads):
        part = wide[:, h * 2 * head_dim : (h + 1) * 2 * head_dim]
        weighted = jnp.where(row_id % heads == h, part, weighted)
    if not first:
        factor = jnp.exp(earlier - highest)
        weighted = weighted + before_ref[pl.ds(0, lines), :] * factor
        totals = totals + before_ref[pl.ds(2 * lines, lines), :][:, :1] * factor
    state_ref[pl.ds(0, lines), :] = weighted
    state_ref[pl.ds(lines, lines), :] = jnp.broadcast_to(highest, (lines, 2 * head_dim))
    state_ref[pl.ds(2 * lines, lines), :] = jnp.broadcast_to(totals, (lines, 2 * head_dim))
    for copy in k_writes + v_writes:
        copy.wait()


def project(name, arrays, pieces, wk, wv, queries, table, heads, head_dim, all_rows, carried):
    depth, columns = wk.shape
    tile = min(256, columns)
    total = sum(piece[2] for piece in pieces)
    lines = max(8, 2 * heads)
    count = len(pieces)
    anywhere = pl.BlockSpec(memory_space=pltpu.HBM)
    vmem = pl.BlockSpec(memory_space=pltpu.VMEM)
    first = carried is None
    operands = [*arrays, wk, wv, queries, table]
    in_specs = [pl.BlockSpec(memory_space=pl.ANY)] * count + [anywhere, anywhere, vmem, vmem]
    aliases = {}
    if not first:
        state, keys, values = carried
        operands += [state, keys, values]
        in_specs += [vmem, anywhere, anywhere]
        aliases = {count + 5: 0, count + 6: 1}
    cache = jax.ShapeDtypeStruct((all_rows, columns), BF16)
    keys, values, state = pl.pallas_call(
        functools.partial(project_kernel, pieces, heads, head_dim, tile, first),
        name=name,
        in_specs=in_specs,
        out_specs=[anywhere, anywhere, vmem],
        out_shape=[cache, cache, jax.ShapeDtypeStruct((3 * lines, 2 * head_dim), F32)],
        input_output_aliases=aliases,
        scratch_shapes=[
            pltpu.VMEM((total, depth), BF16),
            pltpu.VMEM((2 * columns // tile, depth, tile), BF16),
            pltpu.VMEM((total, columns), BF16),
            pltpu.VMEM((total, columns), BF16),
            pltpu.SemaphoreType.DMA((count,)),
            pltpu.SemaphoreType.DMA((2 * columns // tile,)),
            pltpu.SemaphoreType.DMA((2 * count,)),
        ],
        compiler_params=pltpu.CompilerParams(vmem_limit_bytes=32 * 1024 * 1024),
        cost_estimate=pl.CostEstimate(
            flops=4 * total * depth * columns,
            transcendentals=0,
            bytes_accessed=4 * depth * columns + 2 * total * (depth + 2 * columns),
        ),
    )(*operands)
    return state, keys, values


def finish_kernel(groups, heads, head_dim, parts, *refs):
    state_refs = refs[: len(groups)]
    lambda_ref, gain_ref, w_ref = refs[len(groups) : len(groups) + 3]
    outs = refs[len(groups) + 3 : len(groups) + 3 + parts]
    board = refs[-1]
    me = lax.axis_index("tp")
    states = [ref[i] for ref, size in zip(state_refs, groups) for i in range(size)]
    lines = states[0].shape[0] // 3
    highest = functools.reduce(jnp.maximum, [s[lines : 2 * lines] for s in states])
    weighted, totals = 0.0, 0.0
    for s in states:
        factor = jnp.exp(s[lines : 2 * lines] - highest)
        weighted = weighted + s[:lines] * factor
        totals = totals + s[2 * lines :] * factor
    reads = weighted / totals
    diff = reads[:heads] - lambda_ref[...] * reads[heads : 2 * heads]
    mean = jnp.mean(diff * diff, axis=-1, keepdims=True)
    normed = diff * lax.rsqrt(mean + 1e-06) * gain_ref[...]
    headed = jnp.concatenate([normed[h : h + 1] for h in range(heads)], axis=1).astype(BF16)
    width = w_ref.shape[1] // parts
    for b in range(parts):
        board[b] = jnp.dot(
            headed, w_ref[:, pl.ds(b * width, width)], preferred_element_type=F32
        )
    for k in range(parts):
        outs[k][...] = board[lax.rem(me + k, parts)].astype(BF16)


def finish(states, lambdas, gain, out_weight, heads, head_dim, parts):
    vmem = pl.BlockSpec(memory_space=pltpu.VMEM)
    groups = [s.shape[0] for s in states]
    width = out_weight.shape[1] // parts
    return pl.pallas_call(
        functools.partial(finish_kernel, groups, heads, head_dim, parts),
        name="finish",
        in_specs=[vmem] * (len(states) + 3),
        out_specs=[vmem] * parts,
        out_shape=[jax.ShapeDtypeStruct((1, width), BF16)] * parts,
        scratch_shapes=[pltpu.VMEM((parts, 1, width), F32)],
        compiler_params=pltpu.CompilerParams(vmem_limit_bytes=16 * 1024 * 1024),
        cost_estimate=pl.CostEstimate(
            flops=2 * out_weight.size, transcendentals=0, bytes_accessed=2 * out_weight.size
        ),
    )(*states, lambdas, gain, out_weight)


def split_rows(rows):
    last = max(16, rows // 4 // 16 * 16)
    if rows % 16 or rows <= 2 * last:
        return [rows]
    return [rows - last, last]


def on_device(axes, layer_input, key_weight, value_weight, new_queries, lambdas, head_gain, out_weight):
    n_sp, n_tp = axes
    heads = lambdas.shape[0]
    columns = key_weight.shape[1]
    head_dim = columns // (2 * heads)
    own = layer_input[0]
    rows = own.shape[0]
    all_rows = rows * n_tp
    first_position = lax.axis_index("sp") * all_rows
    table = rope_table(first_position, all_rows, head_dim)
    paired = n_tp % 2 == 0

    def send(value, move, axis="tp", size=n_tp):
        return lax.ppermute(value, axis, [(i, move(i)) for i in range(size)])

    chunks = split_rows(rows)
    firsts = [sum(chunks[:i]) for i in range(len(chunks))]
    stride = 2 if paired else 1
    hops = range(stride, n_tp, stride)
    crossed = []
    for row, length in zip(firsts, chunks):
        part = own[row : row + length]
        for hop in hops:
            got = send(part, lambda i, hop=hop: (i + hop) % n_tp)
            crossed.append((got, hop, row, length))
    sides = [(own, lambda me: me, 0, rows, rows)]
    if paired:
        sides.append((send(own, lambda i: i ^ 1), lambda me: me ^ 1, 0, rows, rows))
    stages = [sides]
    for row, length in zip(firsts, chunks):
        stage = []
        for got, hop, at, size in crossed:
            if at != row:
                continue
            stage.append((got, lambda me, hop=hop: lax.rem(me + n_tp - hop, n_tp), row, length, rows))
            if paired:
                relayed = send(got, lambda i: i ^ 1)
                stage.append(
                    (relayed, lambda me, hop=hop: lax.rem((me ^ 1) + n_tp - hop, n_tp), row, length, rows)
                )
        if stage:
            stages.append(stage)
    carried = None
    for index, stage in enumerate(stages):
        carried = project(
            f"project_{index}",
            [piece[0] for piece in stage],
            [piece[1:] for piece in stage],
            key_weight,
            value_weight,
            new_queries,
            table,
            heads,
            head_dim,
            all_rows,
            carried,
        )
    state, keys, values = carried
    state = state[None]
    if n_sp <= 4:
        states = [state] + [
            send(state, lambda i, k=k: (i + k) % n_sp, "sp", n_sp) for k in range(1, n_sp)
        ]
    else:
        states = [lax.all_gather(state, "sp", axis=0, tiled=True)]
    lambda_rows = jnp.broadcast_to(lambdas[:, None], (heads, 2 * head_dim))
    parts = finish(states, lambda_rows, head_gain[None], out_weight, heads, head_dim, n_tp)
    mixed = parts[0].astype(F32)
    for k in range(1, n_tp):
        mixed = mixed + send(parts[k], lambda i, k=k: (i + k) % n_tp).astype(F32)
    return keys[None], values[None], mixed.astype(BF16)


def solution(mesh):
    in_specs = (
        P("gr", ("sp", "tp"), None),
        P(None, "tp"),
        P(None, "tp"),
        P("gr", "tp"),
        P("tp"),
        P(),
        P("tp", None),
    )
    out_specs = (P("gr", "sp", "tp"), P("gr", "sp", "tp"), P("gr", "tp"))
    return jax.shard_map(
        functools.partial(on_device, (mesh.shape["sp"], mesh.shape["tp"])),
        mesh=mesh,
        in_specs=in_specs,
        out_specs=out_specs,
        check_vma=False,
    )
```

```python
import functools

import jax
import jax.numpy as jnp
from jax import lax
from jax.experimental import pallas as pl
from jax.experimental.pallas import tpu as pltpu
from jax.sharding import PartitionSpec as P


LANES = 128
F32 = jnp.float32
BF16 = jnp.bfloat16


def rope_table(first_position, count, head_dim):
    inverse = 1.0 / 10000.0 ** (jnp.arange(0, head_dim, 2, dtype=F32) / head_dim)
    positions = first_position + jnp.arange(count, dtype=jnp.int32)
    angles = positions.astype(F32)[:, None] * inverse[None, :]
    cosine, sine = jnp.cos(angles), jnp.sin(angles)
    return jnp.concatenate([cosine, cosine, -sine, sine], axis=-1)


def turn(rows, table, head_dim):
    half = head_dim // 2
    lane = lax.broadcasted_iota(jnp.int32, rows.shape, 1)
    swapped = pltpu.roll(table, head_dim, 1)
    low = lane < head_dim
    cosine = jnp.where(low, table, swapped)
    sine = jnp.where(low, swapped, table)
    left = pltpu.roll(rows, LANES - half, 1)
    right = pltpu.roll(rows, half, 1)
    turned = jnp.where(lane % head_dim < half, left, right)
    return rows * cosine + turned * sine


def project_kernel(pieces, heads, head_dim, tile, first, *refs):
    count = len(pieces)
    x_refs, refs = refs[:count], refs[count:]
    wk_ref, wv_ref, q_ref, table_ref, refs = refs[0], refs[1], refs[2], refs[3], refs[4:]
    if not first:
        before_ref, refs = refs[0], refs[3:]
    k_out, v_out, state_ref, xs, kbuf, vbuf, o_sem = refs
    me = lax.axis_index("tp")
    block_rows = pieces[0][3]
    columns = wk_ref.shape[1]
    lengths = [piece[2] for piece in pieces]
    starts = [sum(lengths[:i]) for i in range(count)]
    total = sum(lengths)
    offsets = [
        pl.multiple_of(source(me) * block_rows + row, 16) for source, row, _, _ in pieces
    ]
    if count > 1 and total <= xs.shape[0]:
        for i in range(count):
            xs[pl.ds(starts[i], lengths[i]), :] = x_refs[i][...]
        spans = [(xs, 0, total)]
    else:
        spans = [(x_refs[i], starts[i], lengths[i]) for i in range(count)]
    tables = [table_ref[pl.ds(offsets[i], lengths[i]), :] for i in range(count)]
    table = tables[0] if count == 1 else jnp.concatenate(tables, axis=0)

    def writes(buffer, out, base):
        return [
            pltpu.make_async_copy(
                buffer.at[pl.ds(starts[i], lengths[i])],
                out.at[pl.ds(offsets[i], lengths[i])],
                o_sem.at[base + i],
            )
            for i in range(count)
        ]

    for c in range(0, columns, tile):
        for x_ref, row, length in spans:
            raw = jnp.dot(
                x_ref[...], wk_ref[:, pl.ds(c, tile)], preferred_element_type=F32
            )
            for d in range(0, tile, LANES):
                turned = turn(raw[:, d : d + LANES], table[row : row + length], head_dim)
                kbuf[pl.ds(row, length), pl.ds(c + d, LANES)] = turned.astype(BF16)
    k_writes = writes(kbuf, k_out, 0)
    for copy in k_writes:
        copy.start()
    for c in range(0, columns, tile):
        for x_ref, row, length in spans:
            raw = jnp.dot(
                x_ref[...], wv_ref[:, pl.ds(c, tile)], preferred_element_type=F32
            )
            vbuf[pl.ds(row, length), pl.ds(c, tile)] = raw.astype(BF16)
    v_writes = writes(vbuf, v_out, count)
    for copy in v_writes:
        copy.start()

    lines = state_ref.shape[0] // 3
    line = lax.broadcasted_iota(jnp.int32, (lines, columns), 0)
    lane = lax.broadcasted_iota(jnp.int32, (lines, columns), 1)
    mine = lane // head_dim == (line % heads) * 2 + line // heads
    spread = jnp.broadcast_to(q_ref[...].astype(F32), (lines, columns))
    queries = jnp.where(mine, spread, 0.0).astype(BF16)
    scores = lax.dot_general(
        queries, kbuf[...], (((1,), (1,)), ((), ())), preferred_element_type=F32
    )
    scores = scores * head_dim ** (-0.5)
    highest = jnp.max(scores, axis=1, keepdims=True)
    if not first:
        earlier = before_ref[pl.ds(lines, lines), :][:, :1]
        highest = jnp.maximum(highest, earlier)
    weights = jnp.exp(scores - highest)
    totals = jnp.sum(weights, axis=1, keepdims=True)
    coarse = weights.astype(BF16)
    fine = (weights - coarse.astype(F32)).astype(BF16)
    values = vbuf[...]
    wide = jnp.dot(coarse, values, preferred_element_type=F32)
    wide = wide + jnp.dot(fine, values, preferred_element_type=F32)
    row_id = lax.broadcasted_iota(jnp.int32, (lines, 2 * head_dim), 0)
    weighted = jnp.zeros((lines, 2 * head_dim), F32)
    for h in range(heads):
        part = wide[:, h * 2 * head_dim : (h + 1) * 2 * head_dim]
        weighted = jnp.where(row_id % heads == h, part, weighted)
    if not first:
        factor = jnp.exp(earlier - highest)
        weighted = weighted + before_ref[pl.ds(0, lines), :] * factor
        totals = totals + before_ref[pl.ds(2 * lines, lines), :][:, :1] * factor
    state_ref[pl.ds(0, lines), :] = weighted
    state_ref[pl.ds(lines, lines), :] = jnp.broadcast_to(highest, (lines, 2 * head_dim))
    state_ref[pl.ds(2 * lines, lines), :] = jnp.broadcast_to(totals, (lines, 2 * head_dim))
    for copy in k_writes + v_writes:
        copy.wait()


def project(arrays, pieces, wk, wv, queries, table, heads, head_dim, all_rows, carried):
    depth, columns = wk.shape
    tile = min(256, columns)
    total = sum(piece[2] for piece in pieces)
    lines = max(8, 2 * heads)
    count = len(pieces)
    anywhere = pl.BlockSpec(memory_space=pltpu.HBM)
    vmem = pl.BlockSpec(memory_space=pltpu.VMEM)
    first = carried is None
    operands = [*arrays, wk, wv, queries, table]
    in_specs = [vmem] * (count + 4)
    aliases = {}
    if not first:
        state, keys, values = carried
        operands += [state, keys, values]
        in_specs += [vmem, anywhere, anywhere]
        aliases = {count + 5: 0, count + 6: 1}
    cache = jax.ShapeDtypeStruct((all_rows, columns), BF16)
    keys, values, state = pl.pallas_call(
        functools.partial(project_kernel, pieces, heads, head_dim, tile, first),
        in_specs=in_specs,
        out_specs=[anywhere, anywhere, vmem],
        out_shape=[cache, cache, jax.ShapeDtypeStruct((3 * lines, 2 * head_dim), F32)],
        input_output_aliases=aliases,
        scratch_shapes=[
            pltpu.VMEM((min(total, 256) if count > 1 else 16, depth), BF16),
            pltpu.VMEM((total, columns), BF16),
            pltpu.VMEM((total, columns), BF16),
            pltpu.SemaphoreType.DMA((2 * count,)),
        ],
        compiler_params=pltpu.CompilerParams(vmem_limit_bytes=32 * 1024 * 1024),
        cost_estimate=pl.CostEstimate(
            flops=4 * total * depth * columns,
            transcendentals=0,
            bytes_accessed=4 * depth * columns + 2 * total * (depth + 2 * columns),
        ),
    )(*operands)
    return state, keys, values


def finish_kernel(groups, heads, parts, *refs):
    state_refs = refs[: len(groups)]
    lambda_ref, gain_ref, w_ref = refs[len(groups) : len(groups) + 3]
    outs = refs[len(groups) + 3 : len(groups) + 3 + parts]
    board = refs[-1]
    me = lax.axis_index("tp")
    states = [ref[i] for ref, size in zip(state_refs, groups) for i in range(size)]
    lines = states[0].shape[0] // 3
    highest = functools.reduce(jnp.maximum, [s[lines : 2 * lines] for s in states])
    weighted, totals = 0.0, 0.0
    for s in states:
        factor = jnp.exp(s[lines : 2 * lines] - highest)
        weighted = weighted + s[:lines] * factor
        totals = totals + s[2 * lines :] * factor
    reads = weighted / totals
    diff = reads[:heads] - lambda_ref[...] * reads[heads : 2 * heads]
    mean = jnp.mean(diff * diff, axis=-1, keepdims=True)
    normed = diff * lax.rsqrt(mean + 1e-06) * gain_ref[...]
    headed = jnp.concatenate([normed[h : h + 1] for h in range(heads)], axis=1).astype(BF16)
    width = w_ref.shape[1] // parts
    for b in range(parts):
        board[b] = jnp.dot(
            headed, w_ref[:, pl.ds(b * width, width)], preferred_element_type=F32
        )
    for k in range(parts):
        outs[k][...] = board[lax.rem(me + k, parts)].astype(BF16)


def finish(states, lambdas, gain, out_weight, heads, parts):
    vmem = pl.BlockSpec(memory_space=pltpu.VMEM)
    groups = [s.shape[0] for s in states]
    width = out_weight.shape[1] // parts
    return pl.pallas_call(
        functools.partial(finish_kernel, groups, heads, parts),
        name="finish",
        in_specs=[vmem] * (len(states) + 3),
        out_specs=[vmem] * parts,
        out_shape=[jax.ShapeDtypeStruct((1, width), BF16)] * parts,
        scratch_shapes=[pltpu.VMEM((parts, 1, width), F32)],
        compiler_params=pltpu.CompilerParams(vmem_limit_bytes=16 * 1024 * 1024),
        cost_estimate=pl.CostEstimate(
            flops=2 * out_weight.size, transcendentals=0, bytes_accessed=2 * out_weight.size
        ),
    )(*states, lambdas, gain, out_weight)


def split_rows(rows):
    last = max(16, rows // 4 // 16 * 16)
    if rows % 16 or rows <= 2 * last:
        return [rows]
    return [rows - last, last]


def on_device(axes, layer_input, key_weight, value_weight, new_queries, lambdas, head_gain, out_weight):
    n_sp, n_tp = axes
    heads = lambdas.shape[0]
    columns = key_weight.shape[1]
    head_dim = columns // (2 * heads)
    own = layer_input[0]
    rows = own.shape[0]
    all_rows = rows * n_tp
    first_position = lax.axis_index("sp") * all_rows
    table = rope_table(first_position, all_rows, head_dim)
    paired = n_tp % 2 == 0

    def send(value, move, axis="tp", size=n_tp):
        return lax.ppermute(value, axis, [(i, move(i)) for i in range(size)])

    chunks = split_rows(rows)
    firsts = [sum(chunks[:i]) for i in range(len(chunks))]
    stride = 2 if paired else 1
    hops = range(stride, n_tp, stride)
    crossed = []
    for row, length in zip(firsts, chunks):
        part = own[row : row + length]
        for hop in hops:
            got = send(part, lambda i, hop=hop: (i + hop) % n_tp)
            crossed.append((got, hop, row, length))
    sides = [(own, lambda me: me, 0, rows, rows)]
    if paired:
        sides.append((send(own, lambda i: i ^ 1), lambda me: me ^ 1, 0, rows, rows))
    stages = [sides]
    for row, length in zip(firsts, chunks):
        stage = []
        for got, hop, at, size in crossed:
            if at != row:
                continue
            stage.append((got, lambda me, hop=hop: lax.rem(me + n_tp - hop, n_tp), row, length, rows))
            if paired:
                relayed = send(got, lambda i: i ^ 1)
                stage.append(
                    (relayed, lambda me, hop=hop: lax.rem((me ^ 1) + n_tp - hop, n_tp), row, length, rows)
                )
        if stage:
            stages.append(stage)
    carried = None
    for stage in stages:
        carried = project(
            [piece[0] for piece in stage],
            [piece[1:] for piece in stage],
            key_weight,
            value_weight,
            new_queries,
            table,
            heads,
            head_dim,
            all_rows,
            carried,
        )
    state, keys, values = carried
    state = state[None]
    if n_sp <= 4:
        states = [state] + [
            send(state, lambda i, k=k: (i + k) % n_sp, "sp", n_sp) for k in range(1, n_sp)
        ]
    else:
        states = [lax.all_gather(state, "sp", axis=0, tiled=True)]
    lambda_rows = jnp.broadcast_to(lambdas[:, None], (heads, 2 * head_dim))
    parts = finish(states, lambda_rows, head_gain[None], out_weight, heads, n_tp)
    mixed = parts[0].astype(F32)
    for k in range(1, n_tp):
        mixed = mixed + send(parts[k], lambda i, k=k: (i + k) % n_tp).astype(F32)
    return keys[None], values[None], mixed.astype(BF16)


def solution(mesh):
    in_specs = (
        P("gr", ("sp", "tp"), None),
        P(None, "tp"),
        P(None, "tp"),
        P("gr", "tp"),
        P("tp"),
        P(),
        P("tp", None),
    )
    out_specs = (P("gr", "sp", "tp"), P("gr", "sp", "tp"), P("gr", "tp"))

    def body(*arrays):
        return on_device((mesh.shape["sp"], mesh.shape["tp"]), *arrays)

    return jax.shard_map(
        body, mesh=mesh, in_specs=in_specs, out_specs=out_specs, check_vma=False
    )
```

```python
import functools

import jax
import jax.numpy as jnp
from jax import lax
from jax.experimental import pallas as pl
from jax.experimental.pallas import tpu as pltpu
from jax.sharding import PartitionSpec as P


LANES = 128
TILE = 512
MIB = 1024 * 1024
F32 = jnp.float32
BF16 = jnp.bfloat16


def rope_table(first_position, count, head_dim):
    inverse = 1.0 / 10000.0 ** (jnp.arange(0, head_dim, 2, dtype=F32) / head_dim)
    positions = first_position + jnp.arange(count, dtype=jnp.int32)
    angles = positions.astype(F32)[:, None] * inverse[None, :]
    cosine, sine = jnp.cos(angles), jnp.sin(angles)
    return jnp.concatenate([cosine, cosine, -sine, sine], axis=-1)


def turn(rows, table, head_dim):
    half = head_dim // 2
    lane = lax.broadcasted_iota(jnp.int32, rows.shape, 1)
    swapped = pltpu.roll(table, head_dim, 1)
    low = lane < head_dim
    cosine = jnp.where(low, table, swapped)
    sine = jnp.where(low, swapped, table)
    left = pltpu.roll(rows, LANES - half, 1)
    right = pltpu.roll(rows, half, 1)
    turned = jnp.where(lane % head_dim < half, left, right)
    return rows * cosine + turned * sine


def in_vmem(array):
    return pltpu.with_memory_space_constraint(array, pltpu.VMEM)


def cut_kernel(firsts, lengths, x_ref, *refs):
    outs, sem = refs[:-1], refs[-1]
    copies = [
        pltpu.make_async_copy(x_ref.at[pl.ds(row, length)], out, sem.at[i])
        for i, (row, length, out) in enumerate(zip(firsts, lengths, outs))
    ]
    for copy in copies:
        copy.start()
    for copy in copies:
        copy.wait()


def cut(array, firsts, lengths):
    return pl.pallas_call(
        functools.partial(cut_kernel, firsts, lengths),
        in_specs=[pl.BlockSpec(memory_space=pltpu.HBM)],
        out_specs=[pl.BlockSpec(memory_space=pltpu.VMEM)] * len(firsts),
        out_shape=[pltpu.VMEM((n, array.shape[1]), array.dtype) for n in lengths],
        scratch_shapes=[pltpu.SemaphoreType.DMA((len(firsts),))],
        compiler_params=pltpu.CompilerParams(vmem_limit_bytes=MIB),
    )(pltpu.with_memory_space_constraint(array, pltpu.HBM))


def row_offsets(pieces):
    me = lax.axis_index("tp")
    return [pl.multiple_of(source(me) * block + row, 16) for source, row, _, block in pieces]


def write_out(pieces, offsets, buffers, outs, sem):
    copies, at = [], 0
    for offset, (_, _, length, _) in zip(offsets, pieces):
        for buffer, out in zip(buffers, outs):
            copies.append(
                pltpu.make_async_copy(
                    buffer.at[pl.ds(at, length)], out.at[pl.ds(offset, length)], sem.at[len(copies)]
                )
            )
        at += length
    for copy in copies:
        copy.start()
    return copies


def project_kernel(pieces, heads, head_dim, tile, first, last, *refs):
    count = len(pieces)
    x_refs, refs = refs[:count], refs[count:]
    wk_ref, wv_ref, q_ref, table_ref, refs = refs[0], refs[1], refs[2], refs[3], refs[4:]
    if not first:
        before_ref, refs = refs[0], refs[1:]
    if not last:
        if not first:
            refs = refs[2:]
        k_out, v_out, state_ref, xs, kbuf, vbuf, k_sem, v_sem = refs
    else:
        kbuf, vbuf, state_ref, xs = refs
    columns = wk_ref.shape[1]
    lengths = [piece[2] for piece in pieces]
    starts = [sum(lengths[:i]) for i in range(count)]
    total = sum(lengths)
    offsets = row_offsets(pieces)
    if count > 1 and total <= xs.shape[0]:
        for i in range(count):
            xs[pl.ds(starts[i], lengths[i]), :] = x_refs[i][...]
        spans = [(xs, 0, total)]
    else:
        spans = [(x_refs[i], starts[i], lengths[i]) for i in range(count)]
    tables = [table_ref[pl.ds(offsets[i], lengths[i]), :] for i in range(count)]
    table = tables[0] if count == 1 else jnp.concatenate(tables, axis=0)
    copies = []
    for c in range(0, columns, tile):
        for x_ref, row, length in spans:
            raw = jnp.dot(
                x_ref[...], wk_ref[:, pl.ds(c, tile)], preferred_element_type=F32
            )
            for d in range(0, tile, LANES):
                turned = turn(raw[:, d : d + LANES], table[row : row + length], head_dim)
                kbuf[pl.ds(row, length), pl.ds(c + d, LANES)] = turned.astype(BF16)
    if not last:
        copies += write_out(pieces, offsets, [kbuf], [k_out], k_sem)
    for c in range(0, columns, tile):
        for x_ref, row, length in spans:
            raw = jnp.dot(
                x_ref[...], wv_ref[:, pl.ds(c, tile)], preferred_element_type=F32
            )
            vbuf[pl.ds(row, length), pl.ds(c, tile)] = raw.astype(BF16)
    if not last:
        copies += write_out(pieces, offsets, [vbuf], [v_out], v_sem)

    lines = state_ref.shape[0] // 3
    line = lax.broadcasted_iota(jnp.int32, (lines, columns), 0)
    lane = lax.broadcasted_iota(jnp.int32, (lines, columns), 1)
    mine = lane // head_dim == (line % heads) * 2 + line // heads
    spread = jnp.broadcast_to(q_ref[...].astype(F32), (lines, columns))
    queries = jnp.where(mine, spread, 0.0).astype(BF16)
    scores = lax.dot_general(
        queries, kbuf[...], (((1,), (1,)), ((), ())), preferred_element_type=F32
    )
    scores = scores * head_dim ** (-0.5)
    highest = jnp.max(scores, axis=1, keepdims=True)
    if not first:
        earlier = before_ref[pl.ds(lines, lines), :][:, :1]
        highest = jnp.maximum(highest, earlier)
    weights = jnp.exp(scores - highest)
    totals = jnp.sum(weights, axis=1, keepdims=True)
    coarse = weights.astype(BF16)
    fine = (weights - coarse.astype(F32)).astype(BF16)
    values = vbuf[...]
    wide = jnp.dot(coarse, values, preferred_element_type=F32)
    wide = wide + jnp.dot(fine, values, preferred_element_type=F32)
    row_id = lax.broadcasted_iota(jnp.int32, (lines, 2 * head_dim), 0)
    weighted = jnp.zeros((lines, 2 * head_dim), F32)
    for h in range(heads):
        part = wide[:, h * 2 * head_dim : (h + 1) * 2 * head_dim]
        weighted = jnp.where(row_id % heads == h, part, weighted)
    if not first:
        factor = jnp.exp(earlier - highest)
        weighted = weighted + before_ref[pl.ds(0, lines), :] * factor
        totals = totals + before_ref[pl.ds(2 * lines, lines), :][:, :1] * factor
    state_ref[pl.ds(0, lines), :] = weighted
    state_ref[pl.ds(lines, lines), :] = jnp.broadcast_to(highest, (lines, 2 * head_dim))
    state_ref[pl.ds(2 * lines, lines), :] = jnp.broadcast_to(totals, (lines, 2 * head_dim))
    for copy in copies:
        copy.wait()


def project(arrays, pieces, wk, wv, queries, table, heads, head_dim, all_rows, carried, last):
    depth, columns = wk.shape
    total = sum(piece[2] for piece in pieces)
    lines = max(8, 2 * heads)
    count = len(pieces)
    anywhere = pl.BlockSpec(memory_space=pltpu.HBM)
    vmem = pl.BlockSpec(memory_space=pltpu.VMEM)
    first = carried is None
    operands = [in_vmem(a) for a in (*arrays, wk, wv, queries, table)]
    aliases = {}
    if not first:
        operands.append(in_vmem(carried[0]))
    in_specs = [vmem] * len(operands)
    own = [pltpu.VMEM((total, columns), BF16)] * 2
    sems = [pltpu.SemaphoreType.DMA((count,))] * 2
    state_shape = jax.ShapeDtypeStruct((3 * lines, 2 * head_dim), F32)
    if last:
        rows_shape = jax.ShapeDtypeStruct((total, columns), BF16)
        own, sems = [], []
    else:
        rows_shape = jax.ShapeDtypeStruct((all_rows, columns), BF16)
        if not first:
            aliases = {len(operands): 0, len(operands) + 1: 1}
            operands += carried[1:]
            in_specs += [anywhere] * 2
    return pl.pallas_call(
        functools.partial(project_kernel, pieces, heads, head_dim, min(TILE, columns), first, last),
        in_specs=in_specs,
        out_specs=[vmem if last else anywhere] * 2 + [vmem],
        out_shape=[rows_shape, rows_shape, state_shape],
        input_output_aliases=aliases,
        scratch_shapes=[pltpu.VMEM((min(total, 256) if count > 1 else 16, depth), BF16), *own, *sems],
        compiler_params=pltpu.CompilerParams(vmem_limit_bytes=12 * MIB),
        cost_estimate=pl.CostEstimate(
            flops=4 * total * depth * columns,
            transcendentals=0,
            bytes_accessed=4 * depth * columns + 2 * total * (depth + 2 * columns),
        ),
    )(*operands)


def store_kernel(pieces, k_rows, v_rows, k_in, v_in, k_out, v_out, sem):
    copies = write_out(pieces, row_offsets(pieces), [k_rows, v_rows], [k_out, v_out], sem)
    for copy in copies:
        copy.wait()


def store(pieces, k_rows, v_rows, keys, values):
    anywhere = pl.BlockSpec(memory_space=pltpu.HBM)
    vmem = pl.BlockSpec(memory_space=pltpu.VMEM)
    cache = jax.ShapeDtypeStruct(keys.shape, keys.dtype)
    return pl.pallas_call(
        functools.partial(store_kernel, pieces),
        name="store",
        in_specs=[vmem, vmem, anywhere, anywhere],
        out_specs=[anywhere, anywhere],
        out_shape=[cache, cache],
        input_output_aliases={2: 0, 3: 1},
        scratch_shapes=[pltpu.SemaphoreType.DMA((2 * len(pieces),))],
        compiler_params=pltpu.CompilerParams(vmem_limit_bytes=MIB),
    )(k_rows, v_rows, keys, values)


def finish_kernel(groups, heads, parts, moves, *refs):
    state_refs = refs[: len(groups)]
    lambda_ref, gain_ref, w_ref = refs[len(groups) : len(groups) + 3]
    outs = refs[len(groups) + 3 : len(groups) + 3 + parts]
    board = refs[-1]
    me = lax.axis_index("tp")
    states = [ref[i] for ref, size in zip(state_refs, groups) for i in range(size)]
    lines = states[0].shape[0] // 3
    highest = functools.reduce(jnp.maximum, [s[lines : 2 * lines] for s in states])
    weighted, totals = 0.0, 0.0
    for s in states:
        factor = jnp.exp(s[lines : 2 * lines] - highest)
        weighted = weighted + s[:lines] * factor
        totals = totals + s[2 * lines :] * factor
    reads = weighted / totals
    diff = reads[:heads] - lambda_ref[...] * reads[heads : 2 * heads]
    mean = jnp.mean(diff * diff, axis=-1, keepdims=True)
    normed = diff * lax.rsqrt(mean + 1e-06) * gain_ref[...]
    headed = jnp.concatenate([normed[h : h + 1] for h in range(heads)], axis=1).astype(BF16)
    width = w_ref.shape[1] // parts
    for b in range(parts):
        board[b] = jnp.dot(
            headed, w_ref[:, pl.ds(b * width, width)], preferred_element_type=F32
        )
    outs[0][...] = board[me].astype(BF16)
    for out, move in zip(outs[1:], moves):
        out[...] = board[move(me)].astype(BF16)


def finish(states, lambdas, gain, out_weight, heads, parts, moves):
    vmem = pl.BlockSpec(memory_space=pltpu.VMEM)
    groups = [s.shape[0] for s in states]
    width = out_weight.shape[1] // parts
    return pl.pallas_call(
        functools.partial(finish_kernel, groups, heads, parts, moves),
        name="finish",
        in_specs=[vmem] * (len(states) + 3),
        out_specs=[vmem] * parts,
        out_shape=[jax.ShapeDtypeStruct((1, width), BF16)] * parts,
        scratch_shapes=[pltpu.VMEM((parts, 1, width), F32)],
        compiler_params=pltpu.CompilerParams(vmem_limit_bytes=16 * 1024 * 1024),
        cost_estimate=pl.CostEstimate(
            flops=2 * out_weight.size, transcendentals=0, bytes_accessed=2 * out_weight.size
        ),
    )(*[in_vmem(a) for a in (*states, lambdas, gain, out_weight)])


def split_rows(rows):
    first, last = rows // 6 // 16 * 16, rows // 4 // 16 * 16
    if rows % 16 or not first:
        return [rows]
    return [first, rows - first - last, last]


def exchange(count):
    if count & (count - 1) == 0:
        return [lambda i, k=k: i ^ k for k in range(1, count)]
    return [lambda i, k=k: (i + k) % count for k in range(1, count)]


def on_device(axes, layer_input, key_weight, value_weight, new_queries, lambdas, head_gain, out_weight):
    n_sp, n_tp = axes
    heads = lambdas.shape[0]
    columns = key_weight.shape[1]
    head_dim = columns // (2 * heads)
    own = layer_input[0]
    rows = own.shape[0]
    all_rows = rows * n_tp
    first_position = lax.axis_index("sp") * all_rows
    table = rope_table(first_position, all_rows, head_dim)
    paired = n_tp % 2 == 0

    def send(value, move, axis="tp", size=n_tp):
        return lax.ppermute(value, axis, [(i, move(i)) for i in range(size)])

    chunks = split_rows(rows)
    firsts = [sum(chunks[:i]) for i in range(len(chunks))]
    stride = 2 if paired else 1
    hops = range(stride, n_tp, stride)
    cuts = cut(own, firsts[:1], chunks[:1])
    if len(chunks) > 1:
        cuts += cut(own, firsts[1:], chunks[1:])
    crossed = []
    for row, length, part in zip(firsts, chunks, cuts):
        for hop in hops:
            got = send(part, lambda i, hop=hop: (i + hop) % n_tp)
            crossed.append((got, hop, row, length))
    sides = [(own, lambda me: me, 0, rows, rows)]
    if paired:
        sibling = send(own, lambda i: i ^ 1)
        sides.append((sibling, lambda me: me ^ 1, 0, rows, rows))
    stages = [sides]
    for row, length in zip(firsts, chunks):
        stage = []
        for got, hop, at, size in crossed:
            if at != row:
                continue
            stage.append((got, lambda me, hop=hop: lax.rem(me + n_tp - hop, n_tp), row, length, rows))
            if paired:
                relayed = send(got, lambda i: i ^ 1)
                stage.append(
                    (relayed, lambda me, hop=hop: lax.rem((me ^ 1) + n_tp - hop, n_tp), row, length, rows)
                )
        if stage:
            stages.append(stage)
    carried = None
    for index, stage in enumerate(stages):
        last = index > 0 and index == len(stages) - 1
        got = project(
            [piece[0] for piece in stage],
            [piece[1:] for piece in stage],
            key_weight,
            value_weight,
            new_queries,
            table,
            heads,
            head_dim,
            all_rows,
            carried,
            last,
        )
        if last:
            keys, values = carried[1:]
            state = got[2]
        else:
            keys, values, state = got
            carried = (state, keys, values)
    state = state[None]
    if n_sp <= 4:
        states = [state]
        for move in exchange(n_sp):
            states.append(send(state, move, "sp", n_sp))
    else:
        states = [lax.all_gather(state, "sp", axis=0, tiled=True)]
    if len(stages) > 1:
        keys, values = store([piece[1:] for piece in stages[-1]], got[0], got[1], keys, values)
    lambda_rows = jnp.broadcast_to(lambdas[:, None], (heads, 2 * head_dim))
    moves = exchange(n_tp)
    shares = finish(states, lambda_rows, head_gain[None], out_weight, heads, n_tp, moves)
    mixed = shares[0].astype(F32)
    for k, move in enumerate(moves):
        got = send(shares[k + 1], move)
        mixed = mixed + got.astype(F32)
    return keys[None], values[None], mixed.astype(BF16)


def solution(mesh):
    in_specs = (
        P("gr", ("sp", "tp"), None),
        P(None, "tp"),
        P(None, "tp"),
        P("gr", "tp"),
        P("tp"),
        P(),
        P("tp", None),
    )
    out_specs = (P("gr", "sp", "tp"), P("gr", "sp", "tp"), P("gr", "tp"))

    def body(*arrays):
        return on_device((mesh.shape["sp"], mesh.shape["tp"]), *arrays)

    return jax.shard_map(
        body, mesh=mesh, in_specs=in_specs, out_specs=out_specs, check_vma=False
    )
```
